512 devices in a mesh: kv: 64 (over z, y), tp: 8 (over x, core).
Axes of the slice: x: 4, y: 4, z: 16, core: 2. Of those that a mesh axis runs over, the one named last changes fastest.
Arguments:
- tokens: bfloat16 [1024, 2048], P('kv', 'tp'), may hold values from -20 to 20
- attn_gain: bfloat16 [2048], replicated, may hold values from 0.099609375 to 1.8984375
- query_weight: bfloat16 [2048, 1024], P(None, 'tp'), may hold values from -0.125 to 0.125
- key_weight: bfloat16 [2048, 1024], P(None, 'tp'), may hold values from -0.125 to 0.125
- value_weight: bfloat16 [2048, 1024], P(None, 'tp'), may hold values from -0.125 to 0.125
- outgate_weight: bfloat16 [2048, 1024], P(None, 'tp'), may hold values from -0.125 to 0.125
- gate_weight: bfloat16 [2, 8, 2048], replicated, may hold values from -0.125 to 0.125
- forget_bias: float32 [8], replicated, may hold values from -1 to 4
- state_matrix: float32 [1024, 8, 128, 128], P('kv', 'tp'), may hold values from -1.8 to 1.8
- state_norm: float32 [1024, 8, 128], P('kv', 'tp'), may hold values from -1.8 to 1.8
- state_max: float32 [1024, 8], P('kv', 'tp'), may hold values from -1 to 1
- out_weight: bfloat16 [1024, 2048], P(None, 'tp'), may hold values from -0.1875 to 0.1875
- mlp_gain: bfloat16 [2048], P('tp'), may hold values from 0.099609375 to 1.8984375
- up_weight: bfloat16 [2048, 8192], P('tp', 'kv'), may hold values from -0.125 to 0.125
- down_weight: bfloat16 [8192, 2048], P('kv', 'tp'), may hold values from -0.0625 to 0.0625
Outputs:
- result: bfloat16 [1024, 2048], P('kv', 'tp')
- next_matrix: float32 [1024, 8, 128, 128], P('kv', 'tp')
- next_norm: float32 [1024, 8, 128], P('kv', 'tp')
- next_max: float32 [1024, 8], P('kv', 'tp')
The draws below stay inside these ranges and needn't reach their ends.
All inputs are finite; a program needn't handle non-finite values.
Results may differ from the reference program's by a relative error of at most 0.013.
Values may be sent and summed in bfloat16 or wider, within the bound.
No kernel may reach another device: no remote copies, remote signals or barrier semaphores. Data moves between devices by JAX's collectives and lax.ppermute only.
A program may use at most 64 MiB of HBM per device.

```python
import jax
import jax.numpy as jnp
from jax import lax

D = 2048
HEADS = 8
HEAD_DIM = 128
FF = 8192
MIX = 1024
BATCH = 1024


def draw_tokens(key, part):
    column_scale = 1.0 + 3.0 * jnp.arange(D, dtype=jnp.float32) / D
    entries = jnp.clip(jax.random.normal(jax.random.fold_in(key, 13), (BATCH, D), jnp.float32), -5.0, 5.0)
    return (entries * column_scale).astype(jnp.bfloat16)


def block_scale(own_key, dims, pieces, least, largest):
    def one(dim, parts):
        steps = jax.random.uniform(jax.random.fold_in(jax.random.fold_in(own_key, 6), dim), (parts,), jnp.float32, least / len(pieces), largest / len(pieces))
        return jnp.repeat(jnp.exp(steps), dims[dim] // parts).reshape((-1,) + (1,) * (len(dims) - dim - 1))

    gain = one(*pieces[0])
    for cut in pieces[1:]:
        gain = gain * one(*cut)
    return gain


def bell_draw(stream_key, dims, spread, most, cuts=(), kind=jnp.bfloat16):
    level = block_scale(stream_key, dims, cuts, -0.22, 0.18) if cuts else 1.0
    drawn = jax.random.normal(stream_key, dims, jnp.float32) * spread * level
    return jnp.minimum(jnp.maximum(drawn, -most), most).astype(kind)


def setup_inputs(seed: int = 0) -> dict:
    arg_keys = jax.random.split(jax.random.key(seed), 16)
    tokens = draw_tokens(jax.random.fold_in(arg_keys[15], 71), 0)
    attn_gain = jnp.clip(1.0 + 0.18 * jax.random.normal(arg_keys[1], (D,), jnp.float32), 0.099609375, 1.8984375).astype(jnp.bfloat16)
    query_weight = bell_draw(arg_keys[2], (D, MIX), D ** -0.5, 0.125, ((1, 8),))
    key_weight = bell_draw(arg_keys[3], (D, MIX), D ** -0.5, 0.125, ((1, 8),))
    value_weight = bell_draw(arg_keys[4], (D, MIX), D ** -0.5, 0.125, ((1, 8),))
    outgate_weight = bell_draw(arg_keys[5], (D, MIX), D ** -0.5, 0.125, ((1, 8),))
    gate_weight = bell_draw(arg_keys[6], (2, HEADS, D), D ** -0.5, 0.125)
    forget_bias = jnp.clip(jax.random.uniform(arg_keys[7], (HEADS,), jnp.float32, -1.0, 4.0), -1.0, 4.0)
    state_matrix = bell_draw(arg_keys[8], (BATCH, HEADS, HEAD_DIM, HEAD_DIM), 0.3, 1.8, ((0, 64), (1, 8)), jnp.float32)
    state_norm = bell_draw(arg_keys[9], (BATCH, HEADS, HEAD_DIM), 0.3, 1.8, ((0, 64), (1, 8)), jnp.float32)
    state_max = jnp.clip(jax.random.uniform(arg_keys[10], (BATCH, HEADS), jnp.float32, -1.0, 1.0) * block_scale(arg_keys[10], (BATCH, HEADS), ((0, 64), (1, 8)), -0.4, 0.0), -1.0, 1.0)
    out_weight = bell_draw(arg_keys[11], (MIX, D), MIX ** -0.5, 0.1875, ((1, 8),))
    mlp_gain = jnp.clip(1.0 + 0.18 * jax.random.normal(arg_keys[12], (D,), jnp.float32), 0.099609375, 1.8984375).astype(jnp.bfloat16)
    up_weight = bell_draw(arg_keys[13], (D, FF), D ** -0.5, 0.125, ((0, 8), (1, 64)))
    down_weight = bell_draw(arg_keys[14], (FF, D), FF ** -0.5, 0.0625, ((0, 64), (1, 8)))
    return {"tokens": tokens, "attn_gain": attn_gain, "query_weight": query_weight, "key_weight": key_weight, "value_weight": value_weight, "outgate_weight": outgate_weight, "gate_weight": gate_weight, "forget_bias": forget_bias, "state_matrix": state_matrix, "state_norm": state_norm, "state_max": state_max, "out_weight": out_weight, "mlp_gain": mlp_gain, "up_weight": up_weight, "down_weight": down_weight}


epsilon = 1e-06

def reference(tokens, attn_gain, query_weight, key_weight, value_weight, outgate_weight, gate_weight, forget_bias, state_matrix, state_norm, state_max, out_weight, mlp_gain, up_weight, down_weight):
    values = tokens.astype(jnp.float32)
    batch = tokens.shape[0]
    model_width = values.shape[1]
    scale_in = lax.rsqrt(lax.optimization_barrier(jnp.sum(values * values, axis=1)) / model_width + epsilon)
    scaled_in = (values * attn_gain.astype(jnp.float32)).astype(jnp.bfloat16)

    def project(weight):
        return jnp.dot(scaled_in, weight, preferred_element_type=jnp.float32) * scale_in[:, None]
    query_rows = project(query_weight).reshape(batch, HEADS, HEAD_DIM)
    key_rows = (project(key_weight) * HEAD_DIM ** (-0.5)).reshape(batch, HEADS, HEAD_DIM)
    value_rows = project(value_weight).reshape(batch, HEADS, HEAD_DIM)
    outgate = project(outgate_weight).reshape(batch, HEADS, HEAD_DIM)
    gate_rows = gate_weight.reshape(2 * HEADS, model_width)
    gate_pre = jnp.einsum('sd,gd->sg', scaled_in, gate_rows, preferred_element_type=jnp.float32) * scale_in[:, None]
    in_gate = gate_pre[:, :HEADS]
    forget_log = jax.nn.log_sigmoid(gate_pre[:, HEADS:] + forget_bias)
    next_max = jnp.maximum(forget_log + state_max, in_gate)
    kept_share = jnp.exp(forget_log + state_max - next_max)
    admitted = jnp.exp(in_gate - next_max)
    next_matrix = kept_share[:, :, None, None] * state_matrix + admitted[:, :, None, None] * key_rows[:, :, :, None] * value_rows[:, :, None, :]
    next_norm = kept_share[:, :, None] * state_norm + admitted[:, :, None] * key_rows
    numerator = jnp.einsum('shd,shde->she', query_rows, next_matrix, precision=lax.Precision.HIGHEST)
    denominator = lax.optimization_barrier(jnp.sum(query_rows * next_norm, axis=2))
    head_out = numerator / jnp.maximum(jnp.abs(denominator), 1.0)[:, :, None]
    mixed = (head_out * jax.nn.sigmoid(outgate)).reshape(batch, HEADS * HEAD_DIM).astype(jnp.bfloat16)
    attended = jnp.dot(mixed, out_weight, preferred_element_type=jnp.float32)
    residual = (values + attended).astype(jnp.bfloat16)
    res_values = residual.astype(jnp.float32)
    scale_mid = lax.rsqrt(lax.optimization_barrier(jnp.sum(res_values * res_values, axis=1)) / model_width + epsilon)
    scaled_mid = (res_values * mlp_gain.astype(jnp.float32)).astype(jnp.bfloat16)
    up_value = jnp.dot(scaled_mid, up_weight, preferred_element_type=jnp.float32) * scale_mid[:, None]
    hidden = jnp.square(jax.nn.relu(up_value)).astype(jnp.bfloat16)
    result = (res_values + jnp.dot(hidden, down_weight, preferred_element_type=jnp.float32)).astype(jnp.bfloat16)
    return (result, next_matrix, next_norm, next_max)
```

```python
import jax
import jax.numpy as jnp
from jax import lax
from jax.sharding import Mesh
from jax.sharding import PartitionSpec as P

KV = ("z", "y")
TP = ("x", "c")
NEAR = ("z", "c")
epsilon = 1e-06
f32 = jnp.float32
bf16 = jnp.bfloat16


def axis_total(axes):
    axes = axes if isinstance(axes, tuple) else (axes,)
    total = 1
    for name in axes:
        total *= lax.axis_size(name)
    return total


def from_everyone(array, axes):
    return lax.all_to_all(
        jnp.broadcast_to(array[None], (axis_total(axes), *array.shape)), axes, 0, 0, tiled=True
    )


def shifted(array, axis, step):
    size = lax.axis_size(axis)
    return lax.ppermute(array, axis, [(i, (i + step) % size) for i in range(size)])


def gather_columns(array, axes):
    tiles = from_everyone(array, axes)
    count, rows, columns = tiles.shape
    return jnp.moveaxis(tiles, 0, 1).reshape(rows, count * columns)


def body(
    tokens,
    attn_gain,
    query_weight,
    key_weight,
    value_weight,
    outgate_weight,
    gate_weight,
    forget_bias,
    state_matrix,
    state_norm,
    state_max,
    out_weight,
    mlp_gain,
    up_weight,
    down_weight,
):
    sequences = tokens.shape[0]
    head_dim = state_matrix.shape[2]
    model_width = attn_gain.shape[0]
    head = lax.axis_index(TP)

    up_scaled = (up_weight.astype(f32) * mlp_gain.astype(f32)[:, None]).astype(bf16)
    block = jnp.stack([up_scaled, down_weight.T])
    following = shifted(block, "y", 1)
    preceding = shifted(block, "y", -1)
    opposite = shifted(following, "y", 1)
    mixer_own = jnp.stack([block, following, preceding, opposite], 1)
    up_other = shifted(mixer_own[0], "c", 1)
    down_other = shifted(mixer_own[1], "c", 1)
    up_parts = (mixer_own[0], up_other)
    down_parts = (mixer_own[1], down_other)

    gates = lax.dynamic_index_in_dim(gate_weight, head, 1, keepdims=False)
    my_bias = lax.dynamic_index_in_dim(forget_bias, head, 0, keepdims=True)
    values = gather_columns(tokens, TP).astype(f32)
    scaled = (values * attn_gain.astype(f32)).astype(bf16)

    def product(weight):
        return jnp.dot(scaled, weight, preferred_element_type=f32)

    gate_part = jnp.einsum("sd,gd->sg", scaled, gates, preferred_element_type=f32)
    squares = jnp.sum(values * values, axis=1)
    scale_in = lax.rsqrt(squares / model_width + epsilon)[:, None]
    query = product(query_weight) * scale_in
    key = product(key_weight) * scale_in * head_dim ** (-0.5)
    value = product(value_weight) * scale_in
    outgate = product(outgate_weight) * scale_in
    gate_pre = gate_part * scale_in
    in_gate = gate_pre[:, :1]
    forget_log = jax.nn.log_sigmoid(gate_pre[:, 1:] + my_bias)
    next_max = jnp.maximum(forget_log + state_max, in_gate)
    kept = jnp.exp(forget_log + state_max - next_max)
    admitted = jnp.exp(in_gate - next_max)
    next_matrix = (
        kept[:, :, None] * state_matrix[:, 0]
        + (admitted * key)[:, :, None] * value[:, None, :]
    )
    next_norm = kept * state_norm[:, 0] + admitted * key
    numerator = jnp.sum(query[:, :, None] * next_matrix, axis=1)
    denominator = jnp.sum(query * next_norm, axis=1, keepdims=True)
    head_out = numerator / jnp.maximum(jnp.abs(denominator), 1.0)
    mixed = (head_out * jax.nn.sigmoid(outgate)).astype(bf16)
    mixed_full = gather_columns(mixed, TP)
    attended = jnp.dot(mixed_full, out_weight, preferred_element_type=f32)
    residual = (tokens.astype(f32) + attended).astype(bf16)

    cores = lax.axis_size("c")
    near = lax.axis_size("z")
    share = sequences // cores
    columns = residual.shape[1]
    outgoing = jnp.broadcast_to(
        residual.reshape(1, cores, share, columns), (near, cores, share, columns)
    ).reshape(near * cores, share, columns)
    rows = lax.all_to_all(outgoing, NEAR, 0, 0, tiled=True)
    rows = rows.reshape(near, cores, share, columns)
    core = lax.axis_index("c")
    rows = [
        lax.dynamic_index_in_dim(rows, index, 1, keepdims=False).reshape(near * share, columns)
        for index in (core, 1 - core)
    ]
    partial = sum(
        jnp.einsum("rf,zfh->rzh", mine, part, preferred_element_type=f32)
        for mine, part in zip(rows, up_parts)
    )
    partial = partial.reshape(near * share, -1)
    own = sum(jnp.sum(jnp.square(mine.astype(f32)), axis=1) for mine in rows)
    high = own.astype(bf16)
    low = (own - high.astype(f32)).astype(bf16)
    packed = jnp.concatenate(
        [partial.astype(bf16), jnp.pad(jnp.stack([high, low], 1), ((0, 0), (0, 126)))], axis=1
    )
    sums = from_everyone(packed, "x")
    gathered = jnp.sum(sums.astype(f32), axis=0)
    hidden_width = partial.shape[1]
    total = gathered[:, hidden_width : hidden_width + 1] + gathered[:, hidden_width + 1 : hidden_width + 2]
    scale_mid = lax.rsqrt(total / model_width + epsilon)
    hidden = jnp.square(jax.nn.relu(gathered[:, :hidden_width] * scale_mid)).astype(bf16)
    hidden = hidden.reshape(near * share, up_parts[0].shape[0], -1)
    down = [
        jnp.einsum("rzh,zfh->rf", hidden, part, preferred_element_type=f32)
        .astype(bf16)
        .reshape(near, share, columns)
        for part in down_parts
    ]
    first = core == 0
    down = [jnp.where(first, down[0], down[1]), jnp.where(first, down[1], down[0])]
    back = lax.all_to_all(
        jnp.stack(down, 1).reshape(near * cores, share, columns), NEAR, 0, 0, tiled=True
    )
    mixer_out = jnp.sum(back.reshape(near, cores, share, columns).astype(f32), axis=0)
    result = (residual.astype(f32) + mixer_out.reshape(sequences, columns)).astype(bf16)
    return (result, next_matrix[:, None], next_norm[:, None], next_max)


def solution(mesh):
    split = Mesh(
        mesh.devices.reshape(16, 4, 4, 2), ("z", "y", "x", "c")
    )
    placed = (
        P(KV, TP),
        P(),
        P(None, TP),
        P(None, TP),
        P(None, TP),
        P(None, TP),
        P(),
        P(),
        P(KV, TP, None, None),
        P(KV, TP, None),
        P(KV, TP),
        P(None, TP),
        P(TP),
        P(TP, KV),
        P(KV, TP),
    )
    return jax.shard_map(
        body,
        mesh=split,
        in_specs=placed,
        out_specs=(P(KV, TP), P(KV, TP, None, None), P(KV, TP, None), P(KV, TP)),
        check_vma=False,
    )
```

```python
import jax
import jax.numpy as jnp
from jax import lax
from jax.experimental import pallas as pl
from jax.experimental.pallas import tpu as pltpu
from jax.sharding import Mesh
from jax.sharding import PartitionSpec as P

KV = ("z", "y")
TP = ("x", "c")
NEAR = ("z", "c")
epsilon = 1e-06
f32 = jnp.float32
bf16 = jnp.bfloat16
VMEM = pl.BlockSpec(memory_space=pltpu.VMEM)
SMEM = pl.BlockSpec(memory_space=pltpu.SMEM)
HBM = pl.BlockSpec(memory_space=pltpu.HBM)


def shifted(array, axis, step):
    size = lax.axis_size(axis)
    return lax.ppermute(array, axis, [(i, (i + step) % size) for i in range(size)])


def exchanged(array, axes):
    return lax.all_to_all(array, axes, 0, 0, tiled=True)


def matmul(a, b):
    return lax.dot_general(a, b, (((1,), (0,)), ((), ())), preferred_element_type=f32)


def matmul_rows(a, b, precision=None):
    return lax.dot_general(
        a, b, (((1,), (1,)), ((), ())), preferred_element_type=f32, precision=precision
    )


def prepare(
    head_ref,
    bias_ref,
    up_source,
    mlp_gain_source,
    down_source,
    gates_source,
    gain_source,
    norm_source,
    max_source,
    query_source,
    key_source,
    value_source,
    outgate_source,
    state_source,
    query_ref,
    key_ref,
    value_ref,
    outgate_ref,
    state_ref,
    gates_ref,
    small_ref,
    block_ref,
    up_ref,
    mlp_gain_ref,
    down_ref,
    all_gates_ref,
    gain_ref,
    norm_ref,
    max_ref,
    semaphores,
):
    pairs = (
        (up_source, up_ref),
        (mlp_gain_source, mlp_gain_ref),
        (down_source, down_ref),
        (gates_source, all_gates_ref),
        (gain_source, gain_ref),
        (norm_source, norm_ref),
        (max_source, max_ref),
        (query_source, query_ref),
        (key_source, key_ref),
        (value_source, value_ref),
        (outgate_source, outgate_ref),
        (state_source, state_ref),
    )
    copies = [
        pltpu.make_async_copy(source, target, semaphores.at[index])
        for index, (source, target) in enumerate(pairs)
    ]
    for copy in copies:
        copy.start()
    for copy in copies[:7]:
        copy.wait()
    half = mlp_gain_ref.shape[1]
    turned = up_ref[...].astype(f32).T
    gain = mlp_gain_ref[...].astype(f32)
    for index in range(mlp_gain_ref.shape[0]):
        span = slice(index * half, (index + 1) * half)
        block_ref[0, :, span] = (turned[:, span] * gain[index : index + 1]).astype(bf16)
    block_ref[1] = down_ref[...]
    head = head_ref[0]
    for kind in range(2):
        gates_ref[kind : kind + 1] = gate_row(all_gates_ref[kind], head)
    rows = gain_ref.shape[0]
    sequences = norm_ref.shape[0]
    small_ref[:rows] = gain_ref[...].astype(f32)
    small_ref[rows : rows + sequences] = norm_ref[...]
    small_ref[rows + sequences :] = jnp.full(
        (small_ref.shape[0] - rows - sequences, small_ref.shape[1]), bias_ref[head], f32
    )
    small_ref[rows + sequences : rows + sequences + 1, :sequences] = max_ref[...]
    for copy in copies[7:]:
        copy.wait()


def gate_row(gates, head):
    mine = lax.broadcasted_iota(jnp.int32, gates.shape, 0) == head
    return jnp.sum(jnp.where(mine, gates.astype(f32), 0.0), axis=0, keepdims=True)


def cell(
    tiles_ref,
    query_ref,
    key_ref,
    value_ref,
    outgate_ref,
    state_ref,
    gates_ref,
    small_ref,
    mixed_ref,
    next_norm_ref,
    next_max_ref,
    kept_ref,
    added_ref,
    value_out_ref,
):
    tiles, sequences, part = tiles_ref.shape
    width = tiles * part
    dim = query_ref.shape[1]
    accumulated = [jnp.zeros((sequences, dim), f32) for _ in range(4)]
    squares = jnp.zeros((sequences, 1), f32)
    gate_in = jnp.zeros((sequences, 1), f32)
    gate_forget = jnp.zeros((sequences, 1), f32)
    lanes = small_ref.shape[1]
    rows = width // lanes
    gain = small_ref[:rows]
    norm = small_ref[rows : rows + sequences]
    bias = small_ref[rows + sequences + 1 : rows + sequences + 2, :1]
    most = small_ref[rows + sequences : rows + sequences + 1, :sequences]
    for index in range(tiles):
        span = slice(index * part, (index + 1) * part)
        values = tiles_ref[index].astype(f32)
        squares += jnp.sum(values * values, axis=1, keepdims=True)
        row = index * part // lanes
        gains = jnp.concatenate([gain[row + k : row + k + 1] for k in range(part // lanes)], axis=1)
        scaled = (values * gains).astype(bf16)
        wide = scaled.astype(f32)
        gate_in += jnp.sum(wide * gates_ref[0:1, span], axis=1, keepdims=True)
        gate_forget += jnp.sum(wide * gates_ref[1:2, span], axis=1, keepdims=True)
        for slot, weight_ref in enumerate((query_ref, key_ref, value_ref, outgate_ref)):
            accumulated[slot] += matmul(scaled, weight_ref[span, :])
    scale = lax.rsqrt(squares / width + epsilon)
    query = accumulated[0] * scale
    key = accumulated[1] * scale * dim ** (-0.5)
    value = accumulated[2] * scale
    outgate = accumulated[3] * scale
    in_gate = gate_in * scale
    forget_log = jax.nn.log_sigmoid(gate_forget * scale + bias)
    square = (sequences, sequences)
    diagonal = lax.broadcasted_iota(jnp.int32, square, 0) == lax.broadcasted_iota(
        jnp.int32, square, 1
    )
    state_max = jnp.sum(jnp.where(diagonal, most, 0.0), axis=1, keepdims=True)
    carried = forget_log + state_max
    next_max = jnp.maximum(carried, in_gate)
    kept = jnp.exp(carried - next_max)
    admitted = jnp.exp(in_gate - next_max)
    added = admitted * key
    next_norm = kept * norm + added
    next_norm_ref[...] = next_norm
    next_max_ref[...] = jnp.sum(jnp.where(diagonal, next_max, 0.0), axis=0, keepdims=True)
    kept_ref[...] = kept
    added_ref[...] = added
    value_out_ref[...] = value
    denominator = jnp.sum(query * next_norm, axis=1, keepdims=True)
    columns = query.T
    read = jnp.concatenate(
        [
            jnp.sum(columns[:, s : s + 1] * state_ref[s], axis=0, keepdims=True)
            for s in range(sequences)
        ],
        axis=0,
    )
    numerator = kept * read + jnp.sum(query * added, axis=1, keepdims=True) * value
    head_out = numerator / jnp.maximum(jnp.abs(denominator), 1.0)
    mixed = (head_out * jax.nn.sigmoid(outgate)).astype(bf16)
    mixed_ref[...] = jnp.broadcast_to(mixed[None], mixed_ref.shape)


def attend(tiles_ref, weight_ref, tokens_ref, residual_ref, outgoing_ref):
    heads, _, dim = tiles_ref.shape
    total = tokens_ref[...].astype(f32)
    attended = jnp.zeros(total.shape, f32)
    for head in range(heads):
        attended += matmul(tiles_ref[head], weight_ref[head * dim : (head + 1) * dim, :])
    residual = (total + attended).astype(bf16)
    residual_ref[...] = residual
    _, cores, share, columns = outgoing_ref.shape
    outgoing_ref[...] = jnp.broadcast_to(
        residual.reshape(1, cores, share, columns), outgoing_ref.shape
    )


def up(core_ref, rows_ref, own0, own1, own2, own3, other_ref, out_ref):
    core = core_ref[0]
    groups, _, share, columns = rows_ref.shape
    count = groups * share
    mine = rows_ref[:, pl.ds(core, 1)].reshape(count, columns)
    theirs = rows_ref[:, pl.ds(1 - core, 1)].reshape(count, columns)
    hidden = other_ref.shape[1]
    pieces = []
    for index, own in enumerate((own0, own1, own2, own3)):
        pieces.append(
            (matmul_rows(mine, own[0]) + matmul_rows(theirs, other_ref[index])).astype(bf16)
        )
    first = mine.astype(f32)
    second = theirs.astype(f32)
    ones = jnp.ones((16, columns), f32)
    squares = matmul_rows(ones, first * first + second * second, lax.Precision.HIGHEST)
    high = squares.astype(bf16)
    low = (squares - high.astype(f32)).astype(bf16)
    for copy in range(out_ref.shape[0]):
        for index, piece in enumerate(pieces):
            out_ref[copy, :count, index * hidden : (index + 1) * hidden] = piece
        out_ref[copy, count:, :count] = high
        out_ref[copy, count:, count : 2 * count] = low
        out_ref[copy, count:, 2 * count :] = jnp.zeros(
            (16, out_ref.shape[2] - 2 * count), bf16
        )


def down(core_ref, sums_ref, own0, own1, own2, own3, other_ref, out_ref):
    core = core_ref[0]
    groups, cores, share, columns = out_ref.shape
    count = groups * share
    hidden = other_ref.shape[1]
    width = columns * cores * sums_ref.shape[0]
    total = jnp.sum(sums_ref[:, :count, :].astype(f32), axis=0)
    tail = jnp.sum(sums_ref[:, count:, : 2 * count].astype(f32), axis=0)
    squares = (tail[:, :count] + tail[:, count:]).T[:, :1]
    scale = lax.rsqrt(squares / width + epsilon)
    active = jnp.maximum(total * scale, 0.0)
    active = (active * active).astype(bf16)
    mine = jnp.zeros((count, columns), f32)
    theirs = jnp.zeros((count, columns), f32)
    for index, own in enumerate((own0, own1, own2, own3)):
        piece = active[:, index * hidden : (index + 1) * hidden]
        mine += matmul(piece, own[1])
        theirs += matmul(piece, other_ref[index])
    out_ref[:, pl.ds(core, 1)] = mine.astype(bf16).reshape(groups, 1, share, columns)
    out_ref[:, pl.ds(1 - core, 1)] = theirs.astype(bf16).reshape(groups, 1, share, columns)


def call(kernel, shapes, specs, scratch=()):
    return pl.pallas_call(
        kernel,
        out_shape=shapes,
        in_specs=specs,
        out_specs=jax.tree.map(lambda _: VMEM, shapes),
        scratch_shapes=scratch,
        compiler_params=pltpu.CompilerParams(vmem_limit_bytes=8 * 2**20),
        cost_estimate=pl.CostEstimate(flops=1000000, bytes_accessed=1000000, transcendentals=0),
    )


def body(
    tokens,
    attn_gain,
    query_weight,
    key_weight,
    value_weight,
    outgate_weight,
    gate_weight,
    forget_bias,
    state_matrix,
    state_norm,
    state_max,
    out_weight,
    mlp_gain,
    up_weight,
    down_weight,
):
    sequences, columns = tokens.shape
    dim = state_matrix.shape[2]
    head = lax.axis_index(TP).reshape(1)
    core = lax.axis_index("c").reshape(1)
    shape = jax.ShapeDtypeStruct
    parts = lax.axis_size(TP)

    tiles = exchanged(jnp.broadcast_to(tokens[None], (parts, *tokens.shape)), TP)

    sources = (
        up_weight,
        mlp_gain.reshape(-1, dim),
        down_weight,
        gate_weight,
        attn_gain.reshape(-1, dim),
        state_norm[:, 0],
        state_max.reshape(1, -1),
    )
    fetched = (query_weight, key_weight, value_weight, outgate_weight, state_matrix[:, 0])
    *fetched, block = call(
        prepare,
        tuple(shape(array.shape, array.dtype) for array in fetched)
        + (
            shape((2, attn_gain.shape[0]), f32),
            shape((attn_gain.shape[0] // dim + sequences + 8, dim), f32),
            shape((2, *down_weight.shape), bf16),
        ),
        [SMEM, SMEM] + [HBM] * (len(sources) + len(fetched)),
        scratch=[pltpu.VMEM(array.shape, array.dtype) for array in sources]
        + [pltpu.SemaphoreType.DMA((len(sources) + len(fetched),))],
    )(
        head,
        forget_bias,
        *(pltpu.with_memory_space_constraint(array, pltpu.HBM) for array in sources + fetched),
    )
    following = shifted(block, "y", 1)
    preceding = shifted(block, "y", -1)
    opposite = shifted(following, "y", 1)
    own = (block, following, preceding, opposite)
    up_other = shifted(jnp.stack([part[0] for part in own]), "c", 1)
    down_other = shifted(jnp.stack([part[1] for part in own]), "c", 1)

    mixed, next_norm, next_max, kept, added, value = call(
        cell,
        (
            shape((parts, sequences, dim), bf16),
            shape((sequences, dim), f32),
            shape((1, sequences), f32),
            shape((sequences, 1), f32),
            shape((sequences, dim), f32),
            shape((sequences, dim), f32),
        ),
        [VMEM] * 8,
    )(tiles, *fetched)
    next_matrix = (
        kept[:, :, None] * state_matrix[:, 0] + added[:, :, None] * value[:, None, :]
    )
    mixed = exchanged(mixed, TP)

    cores = lax.axis_size("c")
    groups = lax.axis_size("z")
    share = sequences // cores
    residual, outgoing = call(
        attend,
        (shape((sequences, columns), bf16), shape((groups, cores, share, columns), bf16)),
        [VMEM] * 3,
    )(mixed, out_weight, tokens)
    rows = exchanged(outgoing.reshape(groups * cores, share, columns), NEAR)
    count = groups * share
    hidden = down_weight.shape[0] * len(own)
    sums = call(
        up, shape((lax.axis_size("x"), count + 16, hidden), bf16), [SMEM] + [VMEM] * 6
    )(core, rows.reshape(groups, cores, share, columns), *own, up_other)
    sums = exchanged(sums, "x")
    back = call(down, shape((groups, cores, share, columns), bf16), [SMEM] + [VMEM] * 6)(
        core, sums, *own, down_other
    )
    back = exchanged(back.reshape(groups * cores, share, columns), NEAR)
    mixer_out = jnp.sum(back.reshape(groups, cores, share, columns).astype(f32), axis=0)
    result = (residual.astype(f32) + mixer_out.reshape(sequences, columns)).astype(bf16)
    return (result, next_matrix[:, None], next_norm[:, None], next_max.reshape(-1, 1))


def solution(mesh):
    split = Mesh(mesh.devices.reshape(16, 4, 4, 2), ("z", "y", "x", "c"))
    placed = (
        P(KV, TP),
        P(),
        P(None, TP),
        P(None, TP),
        P(None, TP),
        P(None, TP),
        P(),
        P(),
        P(KV, TP, None, None),
        P(KV, TP, None),
        P(KV, TP),
        P(None, TP),
        P(TP),
        P(TP, KV),
        P(KV, TP),
    )
    return jax.shard_map(
        body,
        mesh=split,
        in_specs=placed,
        out_specs=(P(KV, TP), P(KV, TP, None, None), P(KV, TP, None), P(KV, TP)),
        check_vma=False,
    )
```

```python
import jax
import jax.numpy as jnp
from jax import lax
from jax.experimental import pallas as pl
from jax.experimental.pallas import tpu as pltpu
from jax.sharding import Mesh
from jax.sharding import PartitionSpec as P

KV = ("zh", "zl", "y")
TP = ("x", "c")
NEAR = ("zl", "y", "c")
epsilon = 1e-06
f32 = jnp.float32
bf16 = jnp.bfloat16
VMEM = pl.BlockSpec(memory_space=pltpu.VMEM)
SMEM = pl.BlockSpec(memory_space=pltpu.SMEM)
HBM = pl.BlockSpec(memory_space=pltpu.HBM)


def shifted(array, axis, step):
    size = lax.axis_size(axis)
    return lax.ppermute(array, axis, [(i, (i + step) % size) for i in range(size)])


def exchanged(array, axes):
    return lax.all_to_all(array, axes, 0, 0, tiled=True)


def matmul(a, b):
    return lax.dot_general(a, b, (((1,), (0,)), ((), ())), preferred_element_type=f32)


def matmul_rows(a, b, precision=None):
    return lax.dot_general(
        a, b, (((1,), (1,)), ((), ())), preferred_element_type=f32, precision=precision
    )


def prepare(
    head_ref,
    up_source,
    mlp_gain_source,
    down_source,
    gates_source,
    gain_source,
    norm_source,
    max_source,
    bias_source,
    query_source,
    key_source,
    value_source,
    outgate_source,
    out_source,
    query_ref,
    key_ref,
    value_ref,
    outgate_ref,
    out_ref,
    gates_ref,
    small_ref,
    block_ref,
    up_ref,
    mlp_gain_ref,
    down_ref,
    all_gates_ref,
    gain_ref,
    norm_ref,
    max_ref,
    bias_ref,
    semaphores,
):
    pairs = (
        (up_source, up_ref),
        (mlp_gain_source, mlp_gain_ref),
        (down_source, down_ref),
        (gates_source, all_gates_ref),
        (gain_source, gain_ref),
        (norm_source, norm_ref),
        (max_source, max_ref),
        (bias_source, bias_ref),
        (query_source, query_ref),
        (key_source, key_ref),
        (value_source, value_ref),
        (outgate_source, outgate_ref),
        (out_source, out_ref),
    )
    copies = [
        pltpu.make_async_copy(source, target, semaphores.at[index])
        for index, (source, target) in enumerate(pairs)
    ]
    for copy in copies:
        copy.start()
    for copy in copies[:8]:
        copy.wait()
    half = mlp_gain_ref.shape[1]
    turned = up_ref[...].astype(f32).T
    gain = mlp_gain_ref[...].astype(f32)
    for index in range(mlp_gain_ref.shape[0]):
        span = slice(index * half, (index + 1) * half)
        block_ref[0, :, span] = (turned[:, span] * gain[index : index + 1]).astype(bf16)
    block_ref[1] = down_ref[...]
    head = head_ref[0]
    for kind in range(2):
        gates_ref[kind : kind + 1] = gate_row(all_gates_ref[kind], head)
    rows = gain_ref.shape[0]
    sequences = norm_ref.shape[0]
    small_ref[:rows] = gain_ref[...].astype(f32)
    small_ref[rows : rows + sequences] = norm_ref[...]
    mine = lax.broadcasted_iota(jnp.int32, bias_ref.shape, 1) == head
    bias = jnp.sum(jnp.where(mine, bias_ref[...], 0.0), axis=1, keepdims=True)
    small_ref[rows + sequences :] = jnp.broadcast_to(
        bias, (small_ref.shape[0] - rows - sequences, small_ref.shape[1])
    )
    small_ref[rows + sequences : rows + sequences + 1, :sequences] = max_ref[...]
    for copy in copies[8:]:
        copy.wait()


def gate_row(gates, head):
    mine = lax.broadcasted_iota(jnp.int32, gates.shape, 0) == head
    return jnp.sum(jnp.where(mine, gates.astype(f32), 0.0), axis=0, keepdims=True)


def cell(
    tiles_ref,
    query_ref,
    key_ref,
    value_ref,
    outgate_ref,
    state_source,
    gates_ref,
    small_ref,
    mixed_ref,
    next_norm_ref,
    next_max_ref,
    kept_ref,
    added_ref,
    value_out_ref,
    state_ref,
    semaphore,
):
    fetch = pltpu.make_async_copy(state_source, state_ref, semaphore)
    fetch.start()
    tiles, sequences, part = tiles_ref.shape
    width = tiles * part
    dim = query_ref.shape[1]
    accumulated = [jnp.zeros((sequences, dim), f32) for _ in range(4)]
    squares = jnp.zeros((sequences, 1), f32)
    gate_in = jnp.zeros((sequences, 1), f32)
    gate_forget = jnp.zeros((sequences, 1), f32)
    lanes = small_ref.shape[1]
    rows = width // lanes
    gain = small_ref[:rows]
    norm = small_ref[rows : rows + sequences]
    bias = small_ref[rows + sequences + 1 : rows + sequences + 2, :1]
    most = small_ref[rows + sequences : rows + sequences + 1, :sequences]
    for index in range(tiles):
        span = slice(index * part, (index + 1) * part)
        values = tiles_ref[index].astype(f32)
        squares += jnp.sum(values * values, axis=1, keepdims=True)
        row = index * part // lanes
        gains = jnp.concatenate([gain[row + k : row + k + 1] for k in range(part // lanes)], axis=1)
        scaled = (values * gains).astype(bf16)
        wide = scaled.astype(f32)
        gate_in += jnp.sum(wide * gates_ref[0:1, span], axis=1, keepdims=True)
        gate_forget += jnp.sum(wide * gates_ref[1:2, span], axis=1, keepdims=True)
        for slot, weight_ref in enumerate((query_ref, key_ref, value_ref, outgate_ref)):
            accumulated[slot] += matmul(scaled, weight_ref[span, :])
    scale = lax.rsqrt(squares / width + epsilon)
    query = accumulated[0] * scale
    key = accumulated[1] * scale * dim ** (-0.5)
    value = accumulated[2] * scale
    outgate = accumulated[3] * scale
    in_gate = gate_in * scale
    forget_log = jax.nn.log_sigmoid(gate_forget * scale + bias)
    square = (sequences, sequences)
    diagonal = lax.broadcasted_iota(jnp.int32, square, 0) == lax.broadcasted_iota(
        jnp.int32, square, 1
    )
    state_max = jnp.sum(jnp.where(diagonal, most, 0.0), axis=1, keepdims=True)
    carried = forget_log + state_max
    next_max = jnp.maximum(carried, in_gate)
    kept = jnp.exp(carried - next_max)
    admitted = jnp.exp(in_gate - next_max)
    added = admitted * key
    next_norm = kept * norm + added
    next_norm_ref[...] = next_norm
    next_max_ref[...] = jnp.sum(jnp.where(diagonal, next_max, 0.0), axis=0, keepdims=True)
    kept_ref[...] = kept
    added_ref[...] = added
    value_out_ref[...] = value
    denominator = jnp.sum(query * next_norm, axis=1, keepdims=True)
    columns = query.T
    fetch.wait()
    read = jnp.concatenate(
        [
            jnp.sum(columns[:, s : s + 1] * state_ref[s], axis=0, keepdims=True)
            for s in range(sequences)
        ],
        axis=0,
    )
    numerator = kept * read + jnp.sum(query * added, axis=1, keepdims=True) * value
    head_out = numerator / jnp.maximum(jnp.abs(denominator), 1.0)
    mixed = (head_out * jax.nn.sigmoid(outgate)).astype(bf16)
    mixed_ref[...] = jnp.broadcast_to(mixed[None], mixed_ref.shape)


def attend(tiles_ref, weight_ref, tokens_ref, residual_ref, outgoing_ref):
    heads, _, dim = tiles_ref.shape
    total = tokens_ref[...].astype(f32)
    attended = jnp.zeros(total.shape, f32)
    for head in range(heads):
        attended += matmul(tiles_ref[head], weight_ref[head * dim : (head + 1) * dim, :])
    residual = (total + attended).astype(bf16)
    residual_ref[...] = residual
    _, cores, share, columns = outgoing_ref.shape
    outgoing_ref[...] = jnp.broadcast_to(
        residual.reshape(1, cores, share, columns), outgoing_ref.shape
    )


def up(core_ref, rows_ref, own0, own1, own2, own3, other_ref, out_ref):
    core = core_ref[0]
    groups, _, share, columns = rows_ref.shape
    count = groups * share
    mine = rows_ref[:, pl.ds(core, 1)].reshape(count, columns)
    theirs = rows_ref[:, pl.ds(1 - core, 1)].reshape(count, columns)
    hidden = other_ref.shape[1]
    pieces = []
    for index, own in enumerate((own0[0], own1[0], own2[0], own3[...])):
        pieces.append(
            (matmul_rows(mine, own) + matmul_rows(theirs, other_ref[index])).astype(bf16)
        )
    first = mine.astype(f32)
    second = theirs.astype(f32)
    ones = jnp.ones((16, columns), f32)
    squares = matmul_rows(ones, first * first + second * second, lax.Precision.HIGHEST)
    high = squares.astype(bf16)
    low = (squares - high.astype(f32)).astype(bf16)
    for copy in range(out_ref.shape[0]):
        for index, piece in enumerate(pieces):
            out_ref[copy, :count, index * hidden : (index + 1) * hidden] = piece
        out_ref[copy, count:, :count] = high
        out_ref[copy, count:, count : 2 * count] = low
        out_ref[copy, count:, 2 * count :] = jnp.zeros(
            (16, out_ref.shape[2] - 2 * count), bf16
        )


def down(core_ref, sums_ref, own0, own1, own2, own3, other_ref, out_ref):
    core = core_ref[0]
    groups, cores, share, columns = out_ref.shape
    count = groups * share
    hidden = other_ref.shape[1]
    width = columns * cores * sums_ref.shape[0]
    total = jnp.sum(sums_ref[:, :count, :].astype(f32), axis=0)
    tail = jnp.sum(sums_ref[:, count:, : 2 * count].astype(f32), axis=0)
    squares = (tail[:, :count] + tail[:, count:]).T[:, :1]
    scale = lax.rsqrt(squares / width + epsilon)
    active = jnp.maximum(total * scale, 0.0)
    active = (active * active).astype(bf16)
    mine = jnp.zeros((count, columns), f32)
    theirs = jnp.zeros((count, columns), f32)
    for index, own in enumerate((own0[1], own1[1], own2[1], own3[...])):
        piece = active[:, index * hidden : (index + 1) * hidden]
        mine += matmul(piece, own)
        theirs += matmul(piece, other_ref[index])
    out_ref[:, pl.ds(core, 1)] = mine.astype(bf16).reshape(groups, 1, share, columns)
    out_ref[:, pl.ds(1 - core, 1)] = theirs.astype(bf16).reshape(groups, 1, share, columns)


def call(kernel, shapes, specs, scratch=()):
    return pl.pallas_call(
        kernel,
        out_shape=shapes,
        in_specs=specs,
        out_specs=jax.tree.map(lambda _: VMEM, shapes),
        scratch_shapes=scratch,
        compiler_params=pltpu.CompilerParams(vmem_limit_bytes=8 * 2**20),
        cost_estimate=pl.CostEstimate(flops=1000000, bytes_accessed=1000000, transcendentals=0),
    )


def body(
    tokens,
    attn_gain,
    query_weight,
    key_weight,
    value_weight,
    outgate_weight,
    gate_weight,
    forget_bias,
    state_matrix,
    state_norm,
    state_max,
    out_weight,
    mlp_gain,
    up_weight,
    down_weight,
):
    sequences, columns = tokens.shape
    dim = state_matrix.shape[2]
    head = lax.axis_index(TP).reshape(1)
    core = lax.axis_index("c").reshape(1)
    shape = jax.ShapeDtypeStruct
    parts = lax.axis_size(TP)

    tiles = exchanged(jnp.broadcast_to(tokens[None], (parts, *tokens.shape)), TP)

    sources = (
        up_weight,
        mlp_gain.reshape(-1, dim),
        down_weight,
        gate_weight,
        attn_gain.reshape(-1, dim),
        state_norm[:, 0],
        state_max.reshape(1, -1),
        forget_bias.reshape(1, -1),
    )
    fetched = (query_weight, key_weight, value_weight, outgate_weight, out_weight)
    *projections, out_weight, gates, small, block = call(
        prepare,
        tuple(shape(array.shape, array.dtype) for array in fetched)
        + (
            shape((2, attn_gain.shape[0]), f32),
            shape((attn_gain.shape[0] // dim + sequences + 8, dim), f32),
            shape((2, *down_weight.shape), bf16),
        ),
        [SMEM] + [HBM] * (len(sources) + len(fetched)),
        scratch=[pltpu.VMEM(array.shape, array.dtype) for array in sources]
        + [pltpu.SemaphoreType.DMA((len(sources) + len(fetched),))],
    )(
        head,
        *(pltpu.with_memory_space_constraint(array, pltpu.HBM) for array in sources + fetched),
    )
    following = shifted(block, "zh", 1)
    preceding = shifted(block, "zh", -1)
    opposite_up = shifted(following[0], "zh", 1)
    opposite_down = shifted(preceding[1], "zh", -1)
    own = (block, following, preceding)
    up_other = shifted(
        jnp.stack([block[0], following[0], preceding[0], opposite_up]), "c", 1
    )
    down_other = shifted(jnp.stack([block[1], following[1], preceding[1], opposite_down]), "c", 1)

    mixed, next_norm, next_max, kept, added, value = call(
        cell,
        (
            shape((parts, sequences, dim), bf16),
            shape((sequences, dim), f32),
            shape((1, sequences), f32),
            shape((sequences, 1), f32),
            shape((sequences, dim), f32),
            shape((sequences, dim), f32),
        ),
        [VMEM] * 5 + [HBM] + [VMEM] * 2,
        scratch=[pltpu.VMEM((sequences, dim, dim), f32), pltpu.SemaphoreType.DMA],
    )(
        tiles,
        *projections,
        pltpu.with_memory_space_constraint(state_matrix[:, 0], pltpu.HBM),
        gates,
        small,
    )
    next_matrix = (
        kept[:, :, None] * state_matrix[:, 0] + added[:, :, None] * value[:, None, :]
    )
    mixed = exchanged(mixed, TP)

    cores = lax.axis_size("c")
    groups = lax.axis_size("zl") * lax.axis_size("y")
    share = sequences // cores
    residual, outgoing = call(
        attend,
        (shape((sequences, columns), bf16), shape((groups, cores, share, columns), bf16)),
        [VMEM] * 3,
    )(mixed, out_weight, tokens)
    rows = exchanged(outgoing.reshape(groups * cores, share, columns), NEAR)
    count = groups * share
    hidden = down_weight.shape[0] * up_other.shape[0]
    sums = call(
        up, shape((lax.axis_size("x"), count + 16, hidden), bf16), [SMEM] + [VMEM] * 6
    )(core, rows.reshape(groups, cores, share, columns), *own, opposite_up, up_other)
    sums = exchanged(sums, "x")
    back = call(down, shape((groups, cores, share, columns), bf16), [SMEM] + [VMEM] * 6)(
        core, sums, *own, opposite_down, down_other
    )
    back, next_matrix = lax.optimization_barrier((back, next_matrix))
    back = exchanged(back.reshape(groups * cores, share, columns), NEAR)
    mixer_out = jnp.sum(back.reshape(groups, cores, share, columns).astype(f32), axis=0)
    result = (residual.astype(f32) + mixer_out.reshape(sequences, columns)).astype(bf16)
    return (result, next_matrix[:, None], next_norm[:, None], next_max.reshape(-1, 1))


def solution(mesh):
    split = Mesh(mesh.devices.reshape(4, 4, 4, 4, 2), ("zh", "zl", "y", "x", "c"))
    placed = (
        P(KV, TP),
        P(),
        P(None, TP),
        P(None, TP),
        P(None, TP),
        P(None, TP),
        P(),
        P(),
        P(KV, TP, None, None),
        P(KV, TP, None),
        P(KV, TP),
        P(None, TP),
        P(TP),
        P(TP, KV),
        P(KV, TP),
    )
    return jax.shard_map(
        body,
        mesh=split,
        in_specs=placed,
        out_specs=(P(KV, TP), P(KV, TP, None, None), P(KV, TP, None), P(KV, TP)),
        check_vma=False,
    )
```

```python
import jax
import jax.numpy as jnp
from jax import lax
from jax.experimental import pallas as pl
from jax.experimental.pallas import tpu as pltpu
from jax.sharding import Mesh
from jax.sharding import PartitionSpec as P

KV = ("zh", "zl", "y")
TP = ("x", "c")
NEAR = ("zl", "y", "c")
CROSSED = (0, 2, 1, 3)
epsilon = 1e-06
f32 = jnp.float32
bf16 = jnp.bfloat16
VMEM = pl.BlockSpec(memory_space=pltpu.VMEM)
SMEM = pl.BlockSpec(memory_space=pltpu.SMEM)
HBM = pl.BlockSpec(memory_space=pltpu.HBM)


def shifted(array, axis, step):
    size = lax.axis_size(axis)
    return lax.ppermute(array, axis, [(i, (i + step) % size) for i in range(size)])


def crossed(array, step):
    size = lax.axis_size("zh")
    pairs = []
    for plane in range(size):
        pairs.append((2 * plane, 2 * ((plane + step) % size)))
        pairs.append((2 * plane + 1, 2 * ((plane - step) % size) + 1))
    return lax.ppermute(array, ("zh", "c"), pairs)


def exchanged(array, axes):
    return lax.all_to_all(array, axes, 0, 0, tiled=True)


def matmul(a, b):
    return lax.dot_general(a, b, (((1,), (0,)), ((), ())), preferred_element_type=f32)


def matmul_rows(a, b, precision=None):
    return lax.dot_general(
        a, b, (((1,), (1,)), ((), ())), preferred_element_type=f32, precision=precision
    )


def prepare(
    head_ref,
    up_source,
    mlp_gain_source,
    down_source,
    gates_source,
    gain_source,
    norm_source,
    max_source,
    bias_source,
    query_source,
    key_source,
    value_source,
    outgate_source,
    out_source,
    query_ref,
    key_ref,
    value_ref,
    outgate_ref,
    out_ref,
    gates_ref,
    small_ref,
    block_ref,
    up_ref,
    mlp_gain_ref,
    down_ref,
    all_gates_ref,
    gain_ref,
    norm_ref,
    max_ref,
    bias_ref,
    semaphores,
):
    pairs = (
        (up_source, up_ref),
        (mlp_gain_source, mlp_gain_ref),
        (down_source, down_ref),
        (gates_source, all_gates_ref),
        (gain_source, gain_ref),
        (norm_source, norm_ref),
        (max_source, max_ref),
        (bias_source, bias_ref),
        (query_source, query_ref),
        (key_source, key_ref),
        (value_source, value_ref),
        (outgate_source, outgate_ref),
        (out_source, out_ref),
    )
    copies = [
        pltpu.make_async_copy(source, target, semaphores.at[index])
        for index, (source, target) in enumerate(pairs)
    ]
    for copy in copies:
        copy.start()
    for copy in copies[:8]:
        copy.wait()
    half = mlp_gain_ref.shape[1]
    turned = up_ref[...].astype(f32).T
    gain = mlp_gain_ref[...].astype(f32)
    for index in range(mlp_gain_ref.shape[0]):
        span = slice(index * half, (index + 1) * half)
        block_ref[0, :, span] = (turned[:, span] * gain[index : index + 1]).astype(bf16)
    block_ref[1] = down_ref[...]
    head = head_ref[0]
    for kind in range(2):
        gates_ref[kind : kind + 1] = gate_row(all_gates_ref[kind], head)
    rows = gain_ref.shape[0]
    sequences = norm_ref.shape[0]
    small_ref[:rows] = gain_ref[...].astype(f32)
    small_ref[rows : rows + sequences] = norm_ref[...]
    mine = lax.broadcasted_iota(jnp.int32, bias_ref.shape, 1) == head
    bias = jnp.sum(jnp.where(mine, bias_ref[...], 0.0), axis=1, keepdims=True)
    small_ref[rows + sequences :] = jnp.broadcast_to(
        bias, (small_ref.shape[0] - rows - sequences, small_ref.shape[1])
    )
    small_ref[rows + sequences : rows + sequences + 1, :sequences] = max_ref[...]
    for copy in copies[8:]:
        copy.wait()


def gate_row(gates, head):
    mine = lax.broadcasted_iota(jnp.int32, gates.shape, 0) == head
    return jnp.sum(jnp.where(mine, gates.astype(f32), 0.0), axis=0, keepdims=True)


def cell(
    tiles_ref,
    query_ref,
    key_ref,
    value_ref,
    outgate_ref,
    state_source,
    gates_ref,
    small_ref,
    mixed_ref,
    next_norm_ref,
    next_max_ref,
    kept_ref,
    added_ref,
    value_out_ref,
    state_ref,
    semaphores,
):
    step = state_ref.shape[0] // semaphores.shape[0]
    fetches = [
        pltpu.make_async_copy(
            state_source.at[pl.ds(index * step, step)],
            state_ref.at[pl.ds(index * step, step)],
            semaphores.at[index],
        )
        for index in range(semaphores.shape[0])
    ]
    for fetch in fetches:
        fetch.start()
    tiles, sequences, part = tiles_ref.shape
    width = tiles * part
    dim = query_ref.shape[1]
    accumulated = [jnp.zeros((sequences, dim), f32) for _ in range(4)]
    squares = jnp.zeros((sequences, 1), f32)
    gate_in = jnp.zeros((sequences, 1), f32)
    gate_forget = jnp.zeros((sequences, 1), f32)
    lanes = small_ref.shape[1]
    rows = width // lanes
    gain = small_ref[:rows]
    norm = small_ref[rows : rows + sequences]
    bias = small_ref[rows + sequences + 1 : rows + sequences + 2, :1]
    most = small_ref[rows + sequences : rows + sequences + 1, :sequences]
    for index in range(tiles):
        span = slice(index * part, (index + 1) * part)
        values = tiles_ref[index].astype(f32)
        squares += jnp.sum(values * values, axis=1, keepdims=True)
        row = index * part // lanes
        gains = jnp.concatenate([gain[row + k : row + k + 1] for k in range(part // lanes)], axis=1)
        scaled = (values * gains).astype(bf16)
        wide = scaled.astype(f32)
        gate_in += jnp.sum(wide * gates_ref[0:1, span], axis=1, keepdims=True)
        gate_forget += jnp.sum(wide * gates_ref[1:2, span], axis=1, keepdims=True)
        for slot, weight_ref in enumerate((query_ref, key_ref, value_ref, outgate_ref)):
            accumulated[slot] += matmul(scaled, weight_ref[span, :])
    scale = lax.rsqrt(squares / width + epsilon)
    query = accumulated[0] * scale
    key = accumulated[1] * scale * dim ** (-0.5)
    value = accumulated[2] * scale
    outgate = accumulated[3] * scale
    in_gate = gate_in * scale
    forget_log = jax.nn.log_sigmoid(gate_forget * scale + bias)
    square = (sequences, sequences)
    diagonal = lax.broadcasted_iota(jnp.int32, square, 0) == lax.broadcasted_iota(
        jnp.int32, square, 1
    )
    state_max = jnp.sum(jnp.where(diagonal, most, 0.0), axis=1, keepdims=True)
    carried = forget_log + state_max
    next_max = jnp.maximum(carried, in_gate)
    kept = jnp.exp(carried - next_max)
    admitted = jnp.exp(in_gate - next_max)
    added = admitted * key
    next_norm = kept * norm + added
    next_norm_ref[...] = next_norm
    next_max_ref[...] = jnp.sum(jnp.where(diagonal, next_max, 0.0), axis=0, keepdims=True)
    kept_ref[...] = kept
    added_ref[...] = added
    value_out_ref[...] = value
    denominator = jnp.sum(query * next_norm, axis=1, keepdims=True)
    columns = query.T
    for fetch in fetches:
        fetch.wait()
    read = jnp.concatenate(
        [
            jnp.sum(columns[:, s : s + 1] * state_ref[s], axis=0, keepdims=True)
            for s in range(sequences)
        ],
        axis=0,
    )
    numerator = kept * read + jnp.sum(query * added, axis=1, keepdims=True) * value
    head_out = numerator / jnp.maximum(jnp.abs(denominator), 1.0)
    mixed = (head_out * jax.nn.sigmoid(outgate)).astype(bf16)
    mixed_ref[...] = jnp.broadcast_to(mixed[None], mixed_ref.shape)


def attend(tiles_ref, weight_ref, tokens_ref, residual_ref, outgoing_ref):
    heads, _, dim = tiles_ref.shape
    total = tokens_ref[...].astype(f32)
    attended = jnp.zeros(total.shape, f32)
    for head in range(heads):
        attended += matmul(tiles_ref[head], weight_ref[head * dim : (head + 1) * dim, :])
    residual = (total + attended).astype(bf16)
    residual_ref[...] = residual
    _, cores, share, columns = outgoing_ref.shape
    outgoing_ref[...] = jnp.broadcast_to(
        residual.reshape(1, cores, share, columns), outgoing_ref.shape
    )


def up(core_ref, rows_ref, own0, own1, own2, own3, other_ref, out_ref):
    core = core_ref[0]
    groups, _, share, columns = rows_ref.shape
    count = groups * share
    mine = rows_ref[:, pl.ds(core, 1)].reshape(count, columns)
    theirs = rows_ref[:, pl.ds(1 - core, 1)].reshape(count, columns)
    hidden = other_ref.shape[1]
    pieces = []
    for index, own in enumerate((own0[0], own1[0], own2[0], own3[0])):
        pieces.append(
            (matmul_rows(mine, own) + matmul_rows(theirs, other_ref[CROSSED[index]])).astype(bf16)
        )
    first = mine.astype(f32)
    second = theirs.astype(f32)
    ones = jnp.ones((16, columns), f32)
    squares = matmul_rows(ones, first * first + second * second, lax.Precision.HIGHEST)
    high = squares.astype(bf16)
    low = (squares - high.astype(f32)).astype(bf16)
    for copy in range(out_ref.shape[0]):
        for index, piece in enumerate(pieces):
            out_ref[copy, :count, index * hidden : (index + 1) * hidden] = piece
        out_ref[copy, count:, :count] = high
        out_ref[copy, count:, count : 2 * count] = low
        out_ref[copy, count:, 2 * count :] = jnp.zeros(
            (16, out_ref.shape[2] - 2 * count), bf16
        )


def down(core_ref, sums_ref, own0, own1, own2, own3, other_ref, out_ref):
    core = core_ref[0]
    groups, cores, share, columns = out_ref.shape
    count = groups * share
    hidden = other_ref.shape[1]
    width = columns * cores * sums_ref.shape[0]
    total = jnp.sum(sums_ref[:, :count, :].astype(f32), axis=0)
    tail = jnp.sum(sums_ref[:, count:, : 2 * count].astype(f32), axis=0)
    squares = (tail[:, :count] + tail[:, count:]).T[:, :1]
    scale = lax.rsqrt(squares / width + epsilon)
    active = jnp.maximum(total * scale, 0.0)
    active = (active * active).astype(bf16)
    mine = jnp.zeros((count, columns), f32)
    theirs = jnp.zeros((count, columns), f32)
    for index, own in enumerate((own0[1], own1[1], own2[1], own3[1])):
        piece = active[:, index * hidden : (index + 1) * hidden]
        mine += matmul(piece, own)
        theirs += matmul(piece, other_ref[CROSSED[index]])
    out_ref[:, pl.ds(core, 1)] = mine.astype(bf16).reshape(groups, 1, share, columns)
    out_ref[:, pl.ds(1 - core, 1)] = theirs.astype(bf16).reshape(groups, 1, share, columns)


def call(kernel, shapes, specs, scratch=()):
    return pl.pallas_call(
        kernel,
        out_shape=shapes,
        in_specs=specs,
        out_specs=jax.tree.map(lambda _: VMEM, shapes),
        scratch_shapes=scratch,
        compiler_params=pltpu.CompilerParams(vmem_limit_bytes=8 * 2**20),
        cost_estimate=pl.CostEstimate(flops=1000000, bytes_accessed=1000000, transcendentals=0),
    )


def body(
    tokens,
    attn_gain,
    query_weight,
    key_weight,
    value_weight,
    outgate_weight,
    gate_weight,
    forget_bias,
    state_matrix,
    state_norm,
    state_max,
    out_weight,
    mlp_gain,
    up_weight,
    down_weight,
):
    sequences, columns = tokens.shape
    dim = state_matrix.shape[2]
    head = lax.axis_index(TP).reshape(1)
    core = lax.axis_index("c").reshape(1)
    shape = jax.ShapeDtypeStruct
    parts = lax.axis_size(TP)

    tiles = exchanged(jnp.broadcast_to(tokens[None], (parts, *tokens.shape)), TP)

    sources = (
        up_weight,
        mlp_gain.reshape(-1, dim),
        down_weight,
        gate_weight,
        attn_gain.reshape(-1, dim),
        state_norm[:, 0],
        state_max.reshape(1, -1),
        forget_bias.reshape(1, -1),
    )
    fetched = (query_weight, key_weight, value_weight, outgate_weight, out_weight)
    *projections, out_weight, gates, small, block = call(
        prepare,
        tuple(shape(array.shape, array.dtype) for array in fetched)
        + (
            shape((2, attn_gain.shape[0]), f32),
            shape((attn_gain.shape[0] // dim + sequences + 8, dim), f32),
            shape((2, *down_weight.shape), bf16),
        ),
        [SMEM] + [HBM] * (len(sources) + len(fetched)),
        scratch=[pltpu.VMEM(array.shape, array.dtype) for array in sources]
        + [pltpu.SemaphoreType.DMA((len(sources) + len(fetched),))],
    )(
        head,
        *(pltpu.with_memory_space_constraint(array, pltpu.HBM) for array in sources + fetched),
    )
    following = crossed(block, 1)
    preceding = crossed(block, -1)
    opposite = crossed(following, 1)
    own = (block, following, preceding, opposite)
    up_other = shifted(jnp.stack([part[0] for part in own]), "c", 1)
    down_other = shifted(jnp.stack([part[1] for part in own]), "c", 1)

    mixed, next_norm, next_max, kept, added, value = call(
        cell,
        (
            shape((parts, sequences, dim), bf16),
            shape((sequences, dim), f32),
            shape((1, sequences), f32),
            shape((sequences, 1), f32),
            shape((sequences, dim), f32),
            shape((sequences, dim), f32),
        ),
        [VMEM] * 5 + [HBM] + [VMEM] * 2,
        scratch=[pltpu.VMEM((sequences, dim, dim), f32), pltpu.SemaphoreType.DMA((4,))],
    )(
        tiles,
        *projections,
        pltpu.with_memory_space_constraint(state_matrix[:, 0], pltpu.HBM),
        gates,
        small,
    )
    next_matrix = (
        kept[:, :, None] * state_matrix[:, 0] + added[:, :, None] * value[:, None, :]
    )
    mixed = exchanged(mixed, TP)

    cores = lax.axis_size("c")
    groups = lax.axis_size("zl") * lax.axis_size("y")
    share = sequences // cores
    residual, outgoing = call(
        attend,
        (shape((sequences, columns), bf16), shape((groups, cores, share, columns), bf16)),
        [VMEM] * 3,
    )(mixed, out_weight, tokens)
    rows = exchanged(outgoing.reshape(groups * cores, share, columns), NEAR)
    count = groups * share
    hidden = down_weight.shape[0] * up_other.shape[0]
    sums = call(
        up, shape((lax.axis_size("x"), count + 16, hidden), bf16), [SMEM] + [VMEM] * 6
    )(core, rows.reshape(groups, cores, share, columns), *own, up_other)
    sums = exchanged(sums, "x")
    back = call(down, shape((groups, cores, share, columns), bf16), [SMEM] + [VMEM] * 6)(
        core, sums, *own, down_other
    )
    back, next_matrix = lax.optimization_barrier((back, next_matrix))
    back = exchanged(back.reshape(groups * cores, share, columns), NEAR)
    mixer_out = jnp.sum(back.reshape(groups, cores, share, columns).astype(f32), axis=0)
    result = (residual.astype(f32) + mixer_out.reshape(sequences, columns)).astype(bf16)
    return (result, next_matrix[:, None], next_norm[:, None], next_max.reshape(-1, 1))


def solution(mesh):
    split = Mesh(mesh.devices.reshape(4, 4, 4, 4, 2), ("zh", "zl", "y", "x", "c"))
    placed = (
        P(KV, TP),
        P(),
        P(None, TP),
        P(None, TP),
        P(None, TP),
        P(None, TP),
        P(),
        P(),
        P(KV, TP, None, None),
        P(KV, TP, None),
        P(KV, TP),
        P(None, TP),
        P(TP),
        P(TP, KV),
        P(KV, TP),
    )
    return jax.shard_map(
        body,
        mesh=split,
        in_specs=placed,
        out_specs=(P(KV, TP), P(KV, TP, None, None), P(KV, TP, None), P(KV, TP)),
        check_vma=False,
    )
```

```python
import jax
import jax.numpy as jnp
from jax import lax
from jax.experimental import pallas as pl
from jax.experimental.pallas import tpu as pltpu
from jax.sharding import Mesh
from jax.sharding import PartitionSpec as P

KV = ("zh", "zl", "y")
TP = ("x", "c")
NEAR = ("zl", "y", "c")
CROSSED = (0, 2, 1, 3)
epsilon = 1e-06
f32 = jnp.float32
bf16 = jnp.bfloat16
VMEM = pl.BlockSpec(memory_space=pltpu.VMEM)
SMEM = pl.BlockSpec(memory_space=pltpu.SMEM)
HBM = pl.BlockSpec(memory_space=pltpu.HBM)


def shifted(array, axis, step):
    size = lax.axis_size(axis)
    return lax.ppermute(array, axis, [(i, (i + step) % size) for i in range(size)])


def crossed(array, step):
    size = lax.axis_size("zh")
    pairs = []
    for plane in range(size):
        pairs.append((2 * plane, 2 * ((plane + step) % size)))
        pairs.append((2 * plane + 1, 2 * ((plane - step) % size) + 1))
    return lax.ppermute(array, ("zh", "c"), pairs)


def exchanged(array, axes):
    return lax.all_to_all(array, axes, 0, 0, tiled=True)


def matmul(a, b):
    return lax.dot_general(a, b, (((1,), (0,)), ((), ())), preferred_element_type=f32)


def matmul_rows(a, b, precision=None):
    return lax.dot_general(
        a, b, (((1,), (1,)), ((), ())), preferred_element_type=f32, precision=precision
    )


def prepare(
    head_ref,
    up_source,
    mlp_gain_source,
    down_source,
    gates_source,
    gain_source,
    norm_source,
    max_source,
    bias_source,
    query_source,
    key_source,
    value_source,
    outgate_source,
    out_source,
    query_ref,
    key_ref,
    value_ref,
    outgate_ref,
    out_ref,
    gates_ref,
    small_ref,
    block_ref,
    up_ref,
    mlp_gain_ref,
    down_ref,
    all_gates_ref,
    gain_ref,
    norm_ref,
    max_ref,
    bias_ref,
    semaphores,
):
    pairs = (
        (up_source, up_ref),
        (mlp_gain_source, mlp_gain_ref),
        (down_source, down_ref),
        (gates_source, all_gates_ref),
        (gain_source, gain_ref),
        (norm_source, norm_ref),
        (max_source, max_ref),
        (bias_source, bias_ref),
        (query_source, query_ref),
        (key_source, key_ref),
        (value_source, value_ref),
        (outgate_source, outgate_ref),
        (out_source, out_ref),
    )
    copies = [
        pltpu.make_async_copy(source, target, semaphores.at[index])
        for index, (source, target) in enumerate(pairs)
    ]
    for copy in copies:
        copy.start()
    for copy in copies[:8]:
        copy.wait()
    half = mlp_gain_ref.shape[1]
    turned = up_ref[...].astype(f32).T
    gain = mlp_gain_ref[...].astype(f32)
    for index in range(mlp_gain_ref.shape[0]):
        span = slice(index * half, (index + 1) * half)
        block_ref[0, :, span] = (turned[:, span] * gain[index : index + 1]).astype(bf16)
    block_ref[1] = down_ref[...]
    head = head_ref[0]
    for kind in range(2):
        gates_ref[kind : kind + 1] = gate_row(all_gates_ref[kind], head)
    rows = gain_ref.shape[0]
    sequences = norm_ref.shape[0]
    small_ref[:rows] = gain_ref[...].astype(f32)
    small_ref[rows : rows + sequences] = norm_ref[...]
    mine = lax.broadcasted_iota(jnp.int32, bias_ref.shape, 1) == head
    bias = jnp.sum(jnp.where(mine, bias_ref[...], 0.0), axis=1, keepdims=True)
    small_ref[rows + sequences :] = jnp.broadcast_to(
        bias, (small_ref.shape[0] - rows - sequences, small_ref.shape[1])
    )
    small_ref[rows + sequences : rows + sequences + 1, :sequences] = max_ref[...]
    for copy in copies[8:]:
        copy.wait()


def gate_row(gates, head):
    mine = lax.broadcasted_iota(jnp.int32, gates.shape, 0) == head
    return jnp.sum(jnp.where(mine, gates.astype(f32), 0.0), axis=0, keepdims=True)


def cell(
    tiles_ref,
    query_ref,
    key_ref,
    value_ref,
    outgate_ref,
    state_source,
    gates_ref,
    small_ref,
    mixed_ref,
    next_norm_ref,
    next_max_ref,
    kept_ref,
    added_ref,
    value_out_ref,
    state_ref,
    semaphores,
):
    step = state_ref.shape[0] // semaphores.shape[0]
    fetches = [
        pltpu.make_async_copy(
            state_source.at[pl.ds(index * step, step)],
            state_ref.at[pl.ds(index * step, step)],
            semaphores.at[index],
        )
        for index in range(semaphores.shape[0])
    ]
    for fetch in fetches:
        fetch.start()
    tiles, sequences, part = tiles_ref.shape
    width = tiles * part
    dim = query_ref.shape[1]
    accumulated = [jnp.zeros((sequences, dim), f32) for _ in range(4)]
    squares = jnp.zeros((sequences, 1), f32)
    gate_in = jnp.zeros((sequences, 1), f32)
    gate_forget = jnp.zeros((sequences, 1), f32)
    lanes = small_ref.shape[1]
    rows = width // lanes
    gain = small_ref[:rows]
    norm = small_ref[rows : rows + sequences]
    bias = small_ref[rows + sequences + 1 : rows + sequences + 2, :1]
    most = small_ref[rows + sequences : rows + sequences + 1, :sequences]
    for index in range(tiles):
        span = slice(index * part, (index + 1) * part)
        values = tiles_ref[index].astype(f32)
        squares += jnp.sum(values * values, axis=1, keepdims=True)
        row = index * part // lanes
        gains = jnp.concatenate([gain[row + k : row + k + 1] for k in range(part // lanes)], axis=1)
        scaled = (values * gains).astype(bf16)
        wide = scaled.astype(f32)
        gate_in += jnp.sum(wide * gates_ref[0:1, span], axis=1, keepdims=True)
        gate_forget += jnp.sum(wide * gates_ref[1:2, span], axis=1, keepdims=True)
        for slot, weight_ref in enumerate((query_ref, key_ref, value_ref, outgate_ref)):
            accumulated[slot] += matmul(scaled, weight_ref[span, :])
    scale = lax.rsqrt(squares / width + epsilon)
    query = accumulated[0] * scale
    key = accumulated[1] * scale * dim ** (-0.5)
    value = accumulated[2] * scale
    outgate = accumulated[3] * scale
    in_gate = gate_in * scale
    forget_log = jax.nn.log_sigmoid(gate_forget * scale + bias)
    square = (sequences, sequences)
    diagonal = lax.broadcasted_iota(jnp.int32, square, 0) == lax.broadcasted_iota(
        jnp.int32, square, 1
    )
    state_max = jnp.sum(jnp.where(diagonal, most, 0.0), axis=1, keepdims=True)
    carried = forget_log + state_max
    next_max = jnp.maximum(carried, in_gate)
    kept = jnp.exp(carried - next_max)
    admitted = jnp.exp(in_gate - next_max)
    added = admitted * key
    next_norm = kept * norm + added
    next_norm_ref[...] = next_norm
    next_max_ref[...] = jnp.sum(jnp.where(diagonal, next_max, 0.0), axis=0, keepdims=True)
    kept_ref[...] = kept
    added_ref[...] = added
    value_out_ref[...] = value
    denominator = jnp.sum(query * next_norm, axis=1, keepdims=True)
    columns = query.T
    for fetch in fetches:
        fetch.wait()
    read = jnp.concatenate(
        [
            jnp.sum(columns[:, s : s + 1] * state_ref[s], axis=0, keepdims=True)
            for s in range(sequences)
        ],
        axis=0,
    )
    numerator = kept * read + jnp.sum(query * added, axis=1, keepdims=True) * value
    head_out = numerator / jnp.maximum(jnp.abs(denominator), 1.0)
    mixed = (head_out * jax.nn.sigmoid(outgate)).astype(bf16)
    mixed_ref[...] = jnp.broadcast_to(mixed[None], mixed_ref.shape)


def attend(tiles_ref, weight_ref, tokens_ref, residual_ref, outgoing_ref):
    heads, _, dim = tiles_ref.shape
    total = tokens_ref[...].astype(f32)
    attended = jnp.zeros(total.shape, f32)
    for head in range(heads):
        attended += matmul(tiles_ref[head], weight_ref[head * dim : (head + 1) * dim, :])
    residual = (total + attended).astype(bf16)
    residual_ref[...] = residual
    _, cores, share, columns = outgoing_ref.shape
    outgoing_ref[...] = jnp.broadcast_to(
        residual.reshape(1, cores, share, columns), outgoing_ref.shape
    )


def up(core_ref, rows_ref, own0, own1, own2, own3, other_ref, out_ref):
    core = core_ref[0]
    groups, _, share, columns = rows_ref.shape
    count = groups * share
    mine = rows_ref[:, pl.ds(core, 1)].reshape(count, columns)
    theirs = rows_ref[:, pl.ds(1 - core, 1)].reshape(count, columns)
    hidden = other_ref.shape[1]
    pieces = []
    for index, own in enumerate((own0[0], own1[0], own2[0], own3[0])):
        pieces.append(
            (matmul_rows(mine, own) + matmul_rows(theirs, other_ref[CROSSED[index]])).astype(bf16)
        )
    first = mine.astype(f32)
    second = theirs.astype(f32)
    ones = jnp.ones((8, columns), f32)
    squares = matmul_rows(ones, first * first + second * second, lax.Precision.HIGHEST)
    high = squares.astype(bf16)
    low = (squares - high.astype(f32)).astype(bf16)
    for copy in range(out_ref.shape[0]):
        for index, piece in enumerate(pieces):
            out_ref[copy, :count, index * hidden : (index + 1) * hidden] = piece
        out_ref[copy, count:, :count] = high
        out_ref[copy, count:, count : 2 * count] = low
        out_ref[copy, count:, 2 * count :] = jnp.zeros(
            (8, out_ref.shape[2] - 2 * count), bf16
        )


def down(core_ref, sums_ref, own0, own1, own2, own3, other_ref, out_ref):
    core = core_ref[0]
    groups, cores, share, columns = out_ref.shape
    count = groups * share
    hidden = other_ref.shape[1]
    width = columns * cores * sums_ref.shape[0]
    total = jnp.sum(sums_ref[:, :count, :].astype(f32), axis=0)
    tail = jnp.sum(sums_ref[:, count:, : 2 * count].astype(f32), axis=0)
    squares = (tail[:, :count] + tail[:, count:]).T[:, :1]
    scale = lax.rsqrt(squares / width + epsilon)
    active = jnp.maximum(total * scale, 0.0)
    active = (active * active).astype(bf16)
    mine = jnp.zeros((count, columns), f32)
    theirs = jnp.zeros((count, columns), f32)
    for index, own in enumerate((own0[1], own1[1], own2[1], own3[1])):
        piece = active[:, index * hidden : (index + 1) * hidden]
        mine += matmul(piece, own)
        theirs += matmul(piece, other_ref[CROSSED[index]])
    out_ref[:, pl.ds(core, 1)] = mine.astype(bf16).reshape(groups, 1, share, columns)
    out_ref[:, pl.ds(1 - core, 1)] = theirs.astype(bf16).reshape(groups, 1, share, columns)


def call(kernel, shapes, specs, scratch=()):
    return pl.pallas_call(
        kernel,
        out_shape=shapes,
        in_specs=specs,
        out_specs=jax.tree.map(lambda _: VMEM, shapes),
        scratch_shapes=scratch,
        compiler_params=pltpu.CompilerParams(vmem_limit_bytes=8 * 2**20),
        cost_estimate=pl.CostEstimate(flops=1000000, bytes_accessed=1000000, transcendentals=0),
    )


def body(
    tokens,
    attn_gain,
    query_weight,
    key_weight,
    value_weight,
    outgate_weight,
    gate_weight,
    forget_bias,
    state_matrix,
    state_norm,
    state_max,
    out_weight,
    mlp_gain,
    up_weight,
    down_weight,
):
    sequences, columns = tokens.shape
    dim = state_matrix.shape[2]
    head = lax.axis_index(TP).reshape(1)
    core = lax.axis_index("c").reshape(1)
    shape = jax.ShapeDtypeStruct
    parts = lax.axis_size(TP)

    tiles = exchanged(jnp.broadcast_to(tokens[None], (parts, *tokens.shape)), TP)

    sources = (
        up_weight,
        mlp_gain.reshape(-1, dim),
        down_weight,
        gate_weight,
        attn_gain.reshape(-1, dim),
        state_norm[:, 0],
        state_max.reshape(1, -1),
        forget_bias.reshape(1, -1),
    )
    fetched = (query_weight, key_weight, value_weight, outgate_weight, out_weight)
    *projections, out_weight, gates, small, block = call(
        prepare,
        tuple(shape(array.shape, array.dtype) for array in fetched)
        + (
            shape((2, attn_gain.shape[0]), f32),
            shape((attn_gain.shape[0] // dim + sequences + 8, dim), f32),
            shape((2, *down_weight.shape), bf16),
        ),
        [SMEM] + [HBM] * (len(sources) + len(fetched)),
        scratch=[pltpu.VMEM(array.shape, array.dtype) for array in sources]
        + [pltpu.SemaphoreType.DMA((len(sources) + len(fetched),))],
    )(
        head,
        *(pltpu.with_memory_space_constraint(array, pltpu.HBM) for array in sources + fetched),
    )
    following = crossed(block, 1)
    preceding = crossed(block, -1)
    opposite = crossed(following, 1)
    own = (block, following, preceding, opposite)
    up_other = shifted(jnp.stack([part[0] for part in own]), "c", 1)
    down_other = shifted(jnp.stack([part[1] for part in own]), "c", 1)

    mixed, next_norm, next_max, kept, added, value = call(
        cell,
        (
            shape((parts, sequences, dim), bf16),
            shape((sequences, dim), f32),
            shape((1, sequences), f32),
            shape((sequences, 1), f32),
            shape((sequences, dim), f32),
            shape((sequences, dim), f32),
        ),
        [VMEM] * 5 + [HBM] + [VMEM] * 2,
        scratch=[pltpu.VMEM((sequences, dim, dim), f32), pltpu.SemaphoreType.DMA((4,))],
    )(
        tiles,
        *projections,
        pltpu.with_memory_space_constraint(state_matrix[:, 0], pltpu.HBM),
        gates,
        small,
    )
    next_matrix = (
        kept[:, :, None] * state_matrix[:, 0] + added[:, :, None] * value[:, None, :]
    )
    mixed = exchanged(mixed, TP)

    cores = lax.axis_size("c")
    groups = lax.axis_size("zl") * lax.axis_size("y")
    share = sequences // cores
    residual, outgoing = call(
        attend,
        (shape((sequences, columns), bf16), shape((groups, cores, share, columns), bf16)),
        [VMEM] * 3,
    )(mixed, out_weight, tokens)
    rows = exchanged(outgoing.reshape(groups * cores, share, columns), NEAR)
    count = groups * share
    hidden = down_weight.shape[0] * up_other.shape[0]
    sums = call(
        up, shape((lax.axis_size("x"), count + 8, hidden), bf16), [SMEM] + [VMEM] * 6
    )(core, rows.reshape(groups, cores, share, columns), *own, up_other)
    sums = exchanged(sums, "x")
    back = call(down, shape((groups, cores, share, columns), bf16), [SMEM] + [VMEM] * 6)(
        core, sums, *own, down_other
    )
    back, next_matrix = lax.optimization_barrier((back, next_matrix))
    back = exchanged(back.reshape(groups * cores, share, columns), NEAR)
    mixer_out = jnp.sum(back.reshape(groups, cores, share, columns).astype(f32), axis=0)
    result = (residual.astype(f32) + mixer_out.reshape(sequences, columns)).astype(bf16)
    return (result, next_matrix[:, None], next_norm[:, None], next_max.reshape(-1, 1))


def solution(mesh):
    split = Mesh(mesh.devices.reshape(4, 4, 4, 4, 2), ("zh", "zl", "y", "x", "c"))
    placed = (
        P(KV, TP),
        P(),
        P(None, TP),
        P(None, TP),
        P(None, TP),
        P(None, TP),
        P(),
        P(),
        P(KV, TP, None, None),
        P(KV, TP, None),
        P(KV, TP),
        P(None, TP),
        P(TP),
        P(TP, KV),
        P(KV, TP),
    )
    return jax.shard_map(
        body,
        mesh=split,
        in_specs=placed,
        out_specs=(P(KV, TP), P(KV, TP, None, None), P(KV, TP, None), P(KV, TP)),
        check_vma=False,
    )
```

```python
import jax
import jax.numpy as jnp
from jax import lax
from jax.experimental import pallas as pl
from jax.experimental.pallas import tpu as pltpu
from jax.sharding import Mesh
from jax.sharding import PartitionSpec as P

KV = ("zh", "zl", "y")
TP = ("x", "c")
NEAR = ("zl", "y", "c")
CROSSED = (0, 2, 1, 3)
epsilon = 1e-06
f32 = jnp.float32
bf16 = jnp.bfloat16
VMEM = pl.BlockSpec(memory_space=pltpu.VMEM)
SMEM = pl.BlockSpec(memory_space=pltpu.SMEM)
HBM = pl.BlockSpec(memory_space=pltpu.HBM)


def shifted(array, axis, step):
    size = lax.axis_size(axis)
    return lax.ppermute(array, axis, [(i, (i + step) % size) for i in range(size)])


def crossed(array, step):
    size = lax.axis_size("zh")
    pairs = []
    for plane in range(size):
        pairs.append((2 * plane, 2 * ((plane + step) % size)))
        pairs.append((2 * plane + 1, 2 * ((plane - step) % size) + 1))
    return lax.ppermute(array, ("zh", "c"), pairs)


def exchanged(array, axes):
    return lax.all_to_all(array, axes, 0, 0, tiled=True)


def matmul(a, b):
    return lax.dot_general(a, b, (((1,), (0,)), ((), ())), preferred_element_type=f32)


def matmul_rows(a, b, precision=None):
    return lax.dot_general(
        a, b, (((1,), (1,)), ((), ())), preferred_element_type=f32, precision=precision
    )


def prepare(
    head_ref,
    up_source,
    mlp_gain_source,
    down_source,
    gates_source,
    gain_source,
    norm_source,
    max_source,
    bias_source,
    query_source,
    key_source,
    value_source,
    outgate_source,
    out_source,
    state_source,
    query_ref,
    key_ref,
    value_ref,
    outgate_ref,
    out_ref,
    first_ref,
    gates_ref,
    small_ref,
    block_ref,
    up_ref,
    mlp_gain_ref,
    down_ref,
    all_gates_ref,
    gain_ref,
    norm_ref,
    max_ref,
    bias_ref,
    semaphores,
):
    pairs = (
        (up_source, up_ref),
        (mlp_gain_source, mlp_gain_ref),
        (down_source, down_ref),
        (gates_source, all_gates_ref),
        (gain_source, gain_ref),
        (norm_source, norm_ref),
        (max_source, max_ref),
        (bias_source, bias_ref),
        (query_source, query_ref),
        (key_source, key_ref),
        (value_source, value_ref),
        (outgate_source, outgate_ref),
        (out_source, out_ref),
        (state_source.at[pl.ds(0, first_ref.shape[0])], first_ref),
    )
    copies = [
        pltpu.make_async_copy(source, target, semaphores.at[index])
        for index, (source, target) in enumerate(pairs)
    ]
    for copy in copies:
        copy.start()
    for copy in copies[:8]:
        copy.wait()
    half = mlp_gain_ref.shape[1]
    turned = up_ref[...].astype(f32).T
    gain = mlp_gain_ref[...].astype(f32)
    for index in range(mlp_gain_ref.shape[0]):
        span = slice(index * half, (index + 1) * half)
        block_ref[0, :, span] = (turned[:, span] * gain[index : index + 1]).astype(bf16)
    block_ref[1] = down_ref[...]
    head = head_ref[0]
    for kind in range(2):
        gates_ref[kind : kind + 1] = gate_row(all_gates_ref[kind], head)
    rows = gain_ref.shape[0]
    sequences = norm_ref.shape[0]
    small_ref[:rows] = gain_ref[...].astype(f32)
    small_ref[rows : rows + sequences] = norm_ref[...]
    mine = lax.broadcasted_iota(jnp.int32, bias_ref.shape, 1) == head
    bias = jnp.sum(jnp.where(mine, bias_ref[...], 0.0), axis=1, keepdims=True)
    small_ref[rows + sequences :] = jnp.broadcast_to(
        bias, (small_ref.shape[0] - rows - sequences, small_ref.shape[1])
    )
    small_ref[rows + sequences : rows + sequences + 1, :sequences] = max_ref[...]
    for copy in copies[8:]:
        copy.wait()


def gate_row(gates, head):
    mine = lax.broadcasted_iota(jnp.int32, gates.shape, 0) == head
    return jnp.sum(jnp.where(mine, gates.astype(f32), 0.0), axis=0, keepdims=True)


def cell(
    tiles_ref,
    query_ref,
    key_ref,
    value_ref,
    outgate_ref,
    state_source,
    first_ref,
    gates_ref,
    small_ref,
    mixed_ref,
    next_norm_ref,
    next_max_ref,
    kept_ref,
    added_ref,
    value_out_ref,
    state_ref,
    semaphores,
):
    half = first_ref.shape[0]
    step = state_ref.shape[0] // semaphores.shape[0]
    fetches = [
        pltpu.make_async_copy(
            state_source.at[pl.ds(half + index * step, step)],
            state_ref.at[pl.ds(index * step, step)],
            semaphores.at[index],
        )
        for index in range(semaphores.shape[0])
    ]
    for fetch in fetches:
        fetch.start()
    tiles, sequences, part = tiles_ref.shape
    width = tiles * part
    dim = query_ref.shape[1]
    accumulated = [jnp.zeros((sequences, dim), f32) for _ in range(4)]
    squares = jnp.zeros((sequences, 1), f32)
    gate_in = jnp.zeros((sequences, 1), f32)
    gate_forget = jnp.zeros((sequences, 1), f32)
    lanes = small_ref.shape[1]
    rows = width // lanes
    gain = small_ref[:rows]
    norm = small_ref[rows : rows + sequences]
    bias = small_ref[rows + sequences + 1 : rows + sequences + 2, :1]
    most = small_ref[rows + sequences : rows + sequences + 1, :sequences]
    for index in range(tiles):
        span = slice(index * part, (index + 1) * part)
        values = tiles_ref[index].astype(f32)
        squares += jnp.sum(values * values, axis=1, keepdims=True)
        row = index * part // lanes
        gains = jnp.concatenate([gain[row + k : row + k + 1] for k in range(part // lanes)], axis=1)
        scaled = (values * gains).astype(bf16)
        wide = scaled.astype(f32)
        gate_in += jnp.sum(wide * gates_ref[0:1, span], axis=1, keepdims=True)
        gate_forget += jnp.sum(wide * gates_ref[1:2, span], axis=1, keepdims=True)
        for slot, weight_ref in enumerate((query_ref, key_ref, value_ref, outgate_ref)):
            accumulated[slot] += matmul(scaled, weight_ref[span, :])
    scale = lax.rsqrt(squares / width + epsilon)
    query = accumulated[0] * scale
    key = accumulated[1] * scale * dim ** (-0.5)
    value = accumulated[2] * scale
    outgate = accumulated[3] * scale
    in_gate = gate_in * scale
    forget_log = jax.nn.log_sigmoid(gate_forget * scale + bias)
    square = (sequences, sequences)
    diagonal = lax.broadcasted_iota(jnp.int32, square, 0) == lax.broadcasted_iota(
        jnp.int32, square, 1
    )
    state_max = jnp.sum(jnp.where(diagonal, most, 0.0), axis=1, keepdims=True)
    carried = forget_log + state_max
    next_max = jnp.maximum(carried, in_gate)
    kept = jnp.exp(carried - next_max)
    admitted = jnp.exp(in_gate - next_max)
    added = admitted * key
    next_norm = kept * norm + added
    next_norm_ref[...] = next_norm
    next_max_ref[...] = jnp.sum(jnp.where(diagonal, next_max, 0.0), axis=0, keepdims=True)
    kept_ref[...] = kept
    added_ref[...] = added
    value_out_ref[...] = value
    denominator = jnp.sum(query * next_norm, axis=1, keepdims=True)
    columns = query.T
    for fetch in fetches:
        fetch.wait()
    read = jnp.concatenate(
        [
            jnp.sum(
                columns[:, s : s + 1] * (first_ref[s] if s < half else state_ref[s - half]),
                axis=0,
                keepdims=True,
            )
            for s in range(sequences)
        ],
        axis=0,
    )
    numerator = kept * read + jnp.sum(query * added, axis=1, keepdims=True) * value
    head_out = numerator / jnp.maximum(jnp.abs(denominator), 1.0)
    mixed = (head_out * jax.nn.sigmoid(outgate)).astype(bf16)
    mixed_ref[...] = jnp.broadcast_to(mixed[None], mixed_ref.shape)


def attend(tiles_ref, weight_ref, tokens_ref, residual_ref, outgoing_ref):
    heads, _, dim = tiles_ref.shape
    total = tokens_ref[...].astype(f32)
    attended = jnp.zeros(total.shape, f32)
    for head in range(heads):
        attended += matmul(tiles_ref[head], weight_ref[head * dim : (head + 1) * dim, :])
    residual = (total + attended).astype(bf16)
    residual_ref[...] = residual
    _, cores, share, columns = outgoing_ref.shape
    outgoing_ref[...] = jnp.broadcast_to(
        residual.reshape(1, cores, share, columns), outgoing_ref.shape
    )


def up(core_ref, rows_ref, own0, own1, own2, own3, other_ref, out_ref):
    core = core_ref[0]
    groups, _, share, columns = rows_ref.shape
    count = groups * share
    mine = rows_ref[:, pl.ds(core, 1)].reshape(count, columns)
    theirs = rows_ref[:, pl.ds(1 - core, 1)].reshape(count, columns)
    hidden = other_ref.shape[1]
    pieces = []
    for index, own in enumerate((own0[0], own1[0], own2[0], own3[0])):
        pieces.append(
            (matmul_rows(mine, own) + matmul_rows(theirs, other_ref[CROSSED[index]])).astype(bf16)
        )
    first = mine.astype(f32)
    second = theirs.astype(f32)
    ones = jnp.ones((8, columns), f32)
    squares = matmul_rows(ones, first * first + second * second, lax.Precision.HIGHEST)
    high = squares.astype(bf16)
    low = (squares - high.astype(f32)).astype(bf16)
    for copy in range(out_ref.shape[0]):
        for index, piece in enumerate(pieces):
            out_ref[copy, :count, index * hidden : (index + 1) * hidden] = piece
        out_ref[copy, count:, :count] = high
        out_ref[copy, count:, count : 2 * count] = low
        out_ref[copy, count:, 2 * count :] = jnp.zeros(
            (8, out_ref.shape[2] - 2 * count), bf16
        )


def down(core_ref, sums_ref, own0, own1, own2, own3, other_ref, out_ref):
    core = core_ref[0]
    groups, cores, share, columns = out_ref.shape
    count = groups * share
    hidden = other_ref.shape[1]
    width = columns * cores * sums_ref.shape[0]
    total = jnp.sum(sums_ref[:, :count, :].astype(f32), axis=0)
    tail = jnp.sum(sums_ref[:, count:, : 2 * count].astype(f32), axis=0)
    squares = (tail[:, :count] + tail[:, count:]).T[:, :1]
    scale = lax.rsqrt(squares / width + epsilon)
    active = jnp.maximum(total * scale, 0.0)
    active = (active * active).astype(bf16)
    mine = jnp.zeros((count, columns), f32)
    theirs = jnp.zeros((count, columns), f32)
    for index, own in enumerate((own0[1], own1[1], own2[1], own3[1])):
        piece = active[:, index * hidden : (index + 1) * hidden]
        mine += matmul(piece, own)
        theirs += matmul(piece, other_ref[CROSSED[index]])
    out_ref[:, pl.ds(core, 1)] = mine.astype(bf16).reshape(groups, 1, share, columns)
    out_ref[:, pl.ds(1 - core, 1)] = theirs.astype(bf16).reshape(groups, 1, share, columns)


def call(kernel, shapes, specs, scratch=()):
    return pl.pallas_call(
        kernel,
        out_shape=shapes,
        in_specs=specs,
        out_specs=jax.tree.map(lambda _: VMEM, shapes),
        scratch_shapes=scratch,
        compiler_params=pltpu.CompilerParams(vmem_limit_bytes=8 * 2**20),
        cost_estimate=pl.CostEstimate(flops=1000000, bytes_accessed=1000000, transcendentals=0),
    )


def body(
    tokens,
    attn_gain,
    query_weight,
    key_weight,
    value_weight,
    outgate_weight,
    gate_weight,
    forget_bias,
    state_matrix,
    state_norm,
    state_max,
    out_weight,
    mlp_gain,
    up_weight,
    down_weight,
):
    sequences, columns = tokens.shape
    dim = state_matrix.shape[2]
    head = lax.axis_index(TP).reshape(1)
    core = lax.axis_index("c").reshape(1)
    shape = jax.ShapeDtypeStruct
    parts = lax.axis_size(TP)

    tiles = exchanged(jnp.broadcast_to(tokens[None], (parts, *tokens.shape)), TP)

    sources = (
        up_weight,
        mlp_gain.reshape(-1, dim),
        down_weight,
        gate_weight,
        attn_gain.reshape(-1, dim),
        state_norm[:, 0],
        state_max.reshape(1, -1),
        forget_bias.reshape(1, -1),
    )
    fetched = (query_weight, key_weight, value_weight, outgate_weight, out_weight, state_matrix[:, 0])
    *projections, out_weight, first_state, gates, small, block = call(
        prepare,
        tuple(shape(array.shape, array.dtype) for array in fetched[:5])
        + (shape((sequences // 4, dim, dim), f32),)
        + (
            shape((2, attn_gain.shape[0]), f32),
            shape((attn_gain.shape[0] // dim + sequences + 8, dim), f32),
            shape((2, *down_weight.shape), bf16),
        ),
        [SMEM] + [HBM] * (len(sources) + len(fetched)),
        scratch=[pltpu.VMEM(array.shape, array.dtype) for array in sources]
        + [pltpu.SemaphoreType.DMA((len(sources) + len(fetched),))],
    )(
        head,
        *(pltpu.with_memory_space_constraint(array, pltpu.HBM) for array in sources + fetched),
    )
    following = crossed(block, 1)
    preceding = crossed(block, -1)
    opposite = crossed(following, 1)
    own = (block, following, preceding, opposite)
    up_other = shifted(jnp.stack([part[0] for part in own]), "c", 1)
    down_other = shifted(jnp.stack([part[1] for part in own]), "c", 1)

    mixed, next_norm, next_max, kept, added, value = call(
        cell,
        (
            shape((parts, sequences, dim), bf16),
            shape((sequences, dim), f32),
            shape((1, sequences), f32),
            shape((sequences, 1), f32),
            shape((sequences, dim), f32),
            shape((sequences, dim), f32),
        ),
        [VMEM] * 5 + [HBM] + [VMEM] * 3,
        scratch=[pltpu.VMEM((sequences - sequences // 4, dim, dim), f32), pltpu.SemaphoreType.DMA((4,))],
    )(
        tiles,
        *projections,
        pltpu.with_memory_space_constraint(state_matrix[:, 0], pltpu.HBM),
        first_state,
        gates,
        small,
    )
    next_matrix = (
        kept[:, :, None] * state_matrix[:, 0] + added[:, :, None] * value[:, None, :]
    )
    mixed = exchanged(mixed, TP)

    cores = lax.axis_size("c")
    groups = lax.axis_size("zl") * lax.axis_size("y")
    share = sequences // cores
    residual, outgoing = call(
        attend,
        (shape((sequences, columns), bf16), shape((groups, cores, share, columns), bf16)),
        [VMEM] * 3,
    )(mixed, out_weight, tokens)
    rows = exchanged(outgoing.reshape(groups * cores, share, columns), NEAR)
    count = groups * share
    hidden = down_weight.shape[0] * up_other.shape[0]
    sums = call(
        up, shape((lax.axis_size("x"), count + 8, hidden), bf16), [SMEM] + [VMEM] * 6
    )(core, rows.reshape(groups, cores, share, columns), *own, up_other)
    sums = exchanged(sums, "x")
    back = call(down, shape((groups, cores, share, columns), bf16), [SMEM] + [VMEM] * 6)(
        core, sums, *own, down_other
    )
    back, next_matrix = lax.optimization_barrier((back, next_matrix))
    back = exchanged(back.reshape(groups * cores, share, columns), NEAR)
    mixer_out = jnp.sum(back.reshape(groups, cores, share, columns).astype(f32), axis=0)
    result = (residual.astype(f32) + mixer_out.reshape(sequences, columns)).astype(bf16)
    return (result, next_matrix[:, None], next_norm[:, None], next_max.reshape(-1, 1))


def solution(mesh):
    split = Mesh(mesh.devices.reshape(4, 4, 4, 4, 2), ("zh", "zl", "y", "x", "c"))
    placed = (
        P(KV, TP),
        P(),
        P(None, TP),
        P(None, TP),
        P(None, TP),
        P(None, TP),
        P(),
        P(),
        P(KV, TP, None, None),
        P(KV, TP, None),
        P(KV, TP),
        P(None, TP),
        P(TP),
        P(TP, KV),
        P(KV, TP),
    )
    return jax.shard_map(
        body,
        mesh=split,
        in_specs=placed,
        out_specs=(P(KV, TP), P(KV, TP, None, None), P(KV, TP, None), P(KV, TP)),
        check_vma=False,
    )
```
